32 devices in a mesh: sp: 8 (over z, y), tp: 4 (over x, core).
Axes of the slice: x: 2, y: 2, z: 4, core: 2. Of those that a mesh axis runs over, the one named last changes fastest.
Arguments:
- activations: bfloat16 [3584, 2048], P(('sp', 'tp')), may hold values from -27.5 to 27.5
- query_weight: bfloat16 [2048, 2048], P(None, 'tp'), may hold values from -0.088388348 to 0.088388348
- key_weight: bfloat16 [2048, 2048], P(None, 'tp'), may hold values from -0.088388348 to 0.088388348
- value_weight: bfloat16 [2048, 2048], P(None, 'tp'), may hold values from -0.125 to 0.125
- out_weight: bfloat16 [2048, 2048], P('tp'), may hold values from -0.125 to 0.125
- lambdas: float32 [8], P('tp'), may hold values from 0.3 to 0.8
- head_gain: float32 [256], replicated, may hold values from 0.1 to 1.9
Outputs:
- mixed: bfloat16 [3584, 2048], P(('sp', 'tp'))
The draws below stay inside these ranges and needn't reach their ends.
All inputs are finite; a program needn't handle non-finite values.
Results may differ from the reference program's by a relative error of at most 0.014.
Values may be sent and summed in bfloat16 or wider, within the bound.
No kernel may reach another device: no remote copies, remote signals or barrier semaphores. Data moves between devices by JAX's collectives and lax.ppermute only.
A program may use at most 128 MiB of HBM per device.

```python
import jax
import jax.numpy as jnp
from jax import lax

D = 2048
HEADS = 8
HEAD = 128
VALUE = 256
TOK_DEV = 448
SEQ = 3584
N_TP = 4


def draw_activations(key, part):
    noise_base = jnp.clip(jax.random.normal(jax.random.fold_in(key, 1), (SEQ, D), jnp.float32), -4.0, 4.0)
    block_means = jax.random.uniform(jax.random.fold_in(key, 2), (SEQ // TOK_DEV, D), jnp.float32, -1.5, 1.5)
    result = noise_base + jnp.repeat(block_means, TOK_DEV, axis=0)
    return result.astype(jnp.bfloat16)


def paired_weights(key):
    bound_value = 4.0 * D ** (-0.5)
    first_draw = jax.random.normal(jax.random.fold_in(key, 11), (D, HEADS * 2 * HEAD), jnp.float32) * D ** (-0.5)
    second = jax.random.normal(jax.random.fold_in(key, 12), (D, HEADS * 2 * HEAD), jnp.float32) * D ** (-0.5)
    return (first_draw, second, bound_value)


def draw_query_weight(key, part):
    first_draw, second, bound_value = paired_weights(key)
    return jnp.clip(first_draw, -bound_value, bound_value).astype(jnp.bfloat16)


def draw_key_weight(key, part):
    first_draw, second, bound_value = paired_weights(key)
    mixed_draw = second
    return jnp.clip(mixed_draw, -bound_value, bound_value).astype(jnp.bfloat16)


def level_of(key, shape, shards, least, largest):
    gain = 1.0
    for dim, blocks in shards:
        draws = jax.random.uniform(jax.random.fold_in(jax.random.fold_in(key, 6), dim), (blocks,), jnp.float32, least / len(shards), largest / len(shards))
        gain = gain * jnp.repeat(jnp.exp(draws), shape[dim] // blocks).reshape((-1,) + (1,) * (len(shape) - 1 - dim))
    return gain


def bell_draw(stream_key, dims, deviation, reach, split=(), kind=jnp.bfloat16):
    values = jax.random.normal(stream_key, dims, jnp.float32) * deviation
    if len(split) > 0:
        values = level_of(stream_key, dims, split, -0.22, 0.18) * values
    return jnp.clip(values, min=-reach, max=reach).astype(kind)


def setup_inputs(seed: int = 0) -> dict:
    key_of = jax.random.split(jax.random.key(seed), 8)
    activations = draw_activations(jax.random.fold_in(key_of[7], 71), 0)
    query_weight = draw_query_weight(jax.random.fold_in(key_of[7], 71), 0)
    key_weight = draw_key_weight(jax.random.fold_in(key_of[7], 71), 0)
    value_weight = bell_draw(key_of[3], (D, HEADS * VALUE), D ** -0.5, 0.125, ((1, 4),))
    out_weight = bell_draw(key_of[4], (HEADS * VALUE, D), (HEADS * VALUE) ** -0.5, 0.125, ((0, 4),))
    lambdas = jnp.clip(0.3 + 0.5 * jax.random.uniform(key_of[5], (HEADS,), jnp.float32) ** level_of(key_of[5], (HEADS,), ((0, 4),), -0.2, 0.2), 0.3, 0.8)
    head_gain = jnp.clip(1.0 + 0.18 * jax.random.normal(key_of[6], (VALUE,), jnp.float32), 0.1, 1.9)
    return dict(activations=activations, query_weight=query_weight, key_weight=key_weight, value_weight=value_weight, out_weight=out_weight, lambdas=lambdas, head_gain=head_gain)


norm_floor = 0.02

def reference(activations, query_weight, key_weight, value_weight, out_weight, lambdas, head_gain):
    queries = jnp.dot(activations, query_weight, preferred_element_type=jnp.float32).astype(jnp.bfloat16)
    key_rows = jnp.dot(activations, key_weight, preferred_element_type=jnp.float32).astype(jnp.bfloat16)
    value_rows = jnp.dot(activations, value_weight, preferred_element_type=jnp.float32).astype(jnp.bfloat16)
    queries = queries.reshape(SEQ, HEADS, 2, HEAD).transpose(1, 0, 2, 3)
    key_rows = key_rows.reshape(SEQ, HEADS, 2, HEAD).transpose(1, 0, 2, 3)
    value_rows = value_rows.reshape(SEQ, HEADS, VALUE).transpose(1, 0, 2)
    blocks = SEQ // TOK_DEV
    score_scale = HEAD ** (-0.5)
    key_pos = jnp.arange(SEQ, dtype=jnp.int32)

    def one_block(index):
        head_index = index // blocks
        block_index = index % blocks
        first_row = (block_index * TOK_DEV).astype(jnp.int32)
        query_rows = lax.dynamic_slice_in_dim(queries[head_index], first_row, TOK_DEV, 0).astype(jnp.float32)
        key_all = key_rows[head_index].astype(jnp.float32)
        value_all = value_rows[head_index].astype(jnp.float32)
        scores = jnp.einsum('qme,kme->mqk', query_rows, key_all) * score_scale
        query_pos = first_row + jnp.arange(TOK_DEV, dtype=jnp.int32)
        allowed = key_pos[None, :] <= query_pos[:, None]
        masked = jnp.where(allowed[None], scores, -jnp.inf)
        row_top = lax.optimization_barrier(jnp.max(masked, axis=-1, keepdims=True))
        exp_weights = jnp.where(allowed[None], jnp.exp(masked - row_top), 0.0)
        denominators = lax.optimization_barrier(jnp.sum(exp_weights, axis=-1))
        rounded = lax.optimization_barrier(exp_weights.astype(jnp.bfloat16)).astype(jnp.float32)
        weighted = jnp.einsum('mqk,kv->mqv', rounded, value_all)
        lambda_head = lambdas[head_index]
        combined = weighted[0] / denominators[0][:, None] - lambda_head * weighted[1] / denominators[1][:, None]
        inverse_rms = lax.rsqrt(lax.optimization_barrier(jnp.mean(combined * combined, axis=-1, keepdims=True)) + norm_floor)
        return (combined * inverse_rms * head_gain).astype(jnp.bfloat16)
    heads_out = lax.map(one_block, jnp.arange(HEADS * blocks, dtype=jnp.int32))
    heads_out = heads_out.reshape(HEADS, SEQ, VALUE).transpose(1, 0, 2).reshape(SEQ, HEADS * VALUE)
    group_width = HEADS // N_TP * VALUE
    totals = jnp.zeros((SEQ, D), jnp.float32)
    for group_index in range(N_TP):
        columns = heads_out[:, group_index * group_width:(group_index + 1) * group_width]
        weight_rows = out_weight[group_index * group_width:(group_index + 1) * group_width]
        partial_value = jnp.dot(columns, weight_rows, preferred_element_type=jnp.float32).astype(jnp.bfloat16)
        totals = totals + partial_value.astype(jnp.float32)
    return totals.astype(jnp.bfloat16)
```

```python
import functools
import math

import jax
import jax.numpy as jnp
from jax import lax
from jax.experimental import pallas as pl
from jax.experimental.pallas import tpu as pltpu
from jax.sharding import PartitionSpec as P

HEAD = 128
VALUE = 256
MAPS = 2
QK = MAPS * HEAD

norm_floor = 0.02
very_low = -1e30
AXES = ("sp", "tp")


def empty_state(count, local_heads):
    return (
        jnp.full((local_heads, 2, count), very_low, jnp.float32),
        jnp.zeros((local_heads, 2, count), jnp.float32),
        jnp.zeros((local_heads, 2, count, VALUE), jnp.float32),
    )


def absorb(state, query_set, query_pos, key_block, value_block, key_first):
    running, denoms, accums = state
    local_heads = running.shape[0]
    span = key_block.shape[0]
    key_grid = key_block.reshape(span, local_heads, 2, HEAD)
    scores = jnp.einsum(
        "qhme,khme->hmqk", query_set, key_grid, preferred_element_type=jnp.float32
    ) * HEAD ** (-0.5)
    key_pos = key_first + jnp.arange(span, dtype=jnp.int32)
    allowed = key_pos[None, :] <= query_pos[:, None]
    masked = jnp.where(allowed, scores, very_low)
    updated = jnp.maximum(running, jnp.max(masked, axis=-1))
    exp_weights = jnp.where(allowed, jnp.exp(masked - updated[..., None]), 0.0)
    factor = jnp.exp(running - updated)
    denoms = denoms * factor + jnp.sum(exp_weights, axis=-1)
    value_grid = value_block.reshape(span, local_heads, VALUE)
    product = jnp.einsum(
        "hmqk,khv->hmqv",
        exp_weights.astype(jnp.bfloat16),
        value_grid,
        preferred_element_type=jnp.float32,
    )
    accums = accums * factor[..., None] + product
    return (updated, denoms, accums)


def gathered_plan(activations, query_weight, key_weight, value_weight, out_weight, lambdas, head_gain):
    local_heads = lambdas.shape[0]
    query_width = query_weight.shape[1]
    joined_weight = jnp.concatenate([query_weight, key_weight, value_weight], axis=1)
    projected = jnp.dot(
        lax.all_gather(activations, "tp", axis=0, tiled=True),
        joined_weight,
        preferred_element_type=jnp.float32,
    ).astype(jnp.bfloat16)
    row_count = projected.shape[0]
    queries = projected[:, :query_width].reshape(row_count, local_heads, 2, HEAD)
    position = lax.axis_index("sp") * row_count + jnp.arange(row_count, dtype=jnp.int32)
    key_piece = lax.all_gather(projected[:, query_width : 2 * query_width], "sp", axis=0, tiled=True)
    value_piece = lax.all_gather(projected[:, 2 * query_width :], "sp", axis=0, tiled=True)
    length = key_piece.shape[0]
    span = math.gcd(length, 512)

    def one_span(span_index, state):
        offset = span_index * span
        key_block = lax.dynamic_slice_in_dim(key_piece, offset, span, 0)
        value_block = lax.dynamic_slice_in_dim(value_piece, offset, span, 0)
        return lax.cond(
            offset <= position[-1],
            lambda current: absorb(current, queries, position, key_block, value_block, offset),
            lambda current: current,
            state,
        )

    running, denoms, accums = lax.fori_loop(
        0, length // span, one_span, empty_state(row_count, local_heads)
    )
    combined = (
        accums[:, 0] / denoms[:, 0, :, None]
        - lambdas[:, None, None] * accums[:, 1] / denoms[:, 1, :, None]
    )
    inverse_rms = lax.rsqrt(jnp.mean(combined * combined, axis=-1, keepdims=True) + norm_floor)
    normed = (combined * inverse_rms * head_gain).astype(jnp.bfloat16)
    heads_out = jnp.transpose(normed, (1, 0, 2)).reshape(row_count, local_heads * VALUE)
    return lax.psum_scatter(
        jnp.dot(heads_out, out_weight, preferred_element_type=jnp.float32).astype(jnp.bfloat16),
        "tp",
        scatter_dimension=0,
        tiled=True,
    )


TP, MEM, PLANE, CORE, CHIP = range(5)


def project(scalars, pieces, weights, members, reach):
    count = len(pieces)
    rows, depth = pieces[0].shape
    widths = [w.shape[1] // members for w in weights]
    total = sum(widths)

    def kernel(sc, *refs):
        piece_refs = refs[:count]
        weight_refs = refs[count : count + len(weights)]
        outs = refs[count + len(weights) : count + len(weights) + members]
        block, sems = refs[-2:]
        step = pl.program_id(0)

        @pl.when(sc[PLANE] >= reach)
        def _():
            @pl.when(step == 0)
            def _():
                copies = []
                for j in range(count):
                    slot = jnp.bitwise_xor(sc[TP], j)
                    place = pl.ds(pl.multiple_of(slot * rows, 16), rows)
                    copies.append(pltpu.make_async_copy(piece_refs[j], block.at[place], sems.at[j]))
                for copy in copies:
                    copy.start()
                for copy in copies:
                    copy.wait()

            first = 0
            for w, width in zip(weight_refs, widths):
                product = jnp.dot(
                    block[...], w[...], preferred_element_type=jnp.float32
                ).astype(jnp.bfloat16)
                for d in range(members):

                    @pl.when(step == (d - 1) % members)
                    def _():
                        outs[d][:, first : first + width] = product

                first += width

    def head_of(step, sc):
        return (0, lax.rem(sc[MEM] + 1 + step, members))

    shape = (count * rows, total)
    return pl.pallas_call(
        kernel,
        grid_spec=pltpu.PrefetchScalarGridSpec(
            num_scalar_prefetch=1,
            grid=(members,),
            in_specs=[pl.BlockSpec(memory_space=pl.ANY)] * count
            + [pl.BlockSpec((depth, width), head_of) for width in widths],
            out_specs=[pl.BlockSpec(shape, lambda step, sc: (0, 0))] * members,
            scratch_shapes=[
                pltpu.VMEM((count * rows, depth), jnp.bfloat16),
                pltpu.SemaphoreType.DMA((count,)),
            ],
        ),
        out_shape=[jax.ShapeDtypeStruct(shape, jnp.bfloat16)] * members,
        compiler_params=pltpu.CompilerParams(vmem_limit_bytes=40 * 2**20),
        cost_estimate=pl.CostEstimate(
            flops=2 * shape[0] * total * members * depth,
            bytes_accessed=2 * depth * (shape[0] + total * members),
            transcendentals=0,
        ),
        name="project",
    )(scalars, *pieces, *weights)


def attend(scalars, query_parts, blocks, state, finish):
    members = len(query_parts)
    rows = query_parts[0].shape[0]
    plane_rows = members * rows
    tile = plane_rows // 4
    scale = HEAD ** (-0.5) * math.log2(math.e)
    n_kv = len(blocks)

    def kernel(sc, *refs):
        refs = list(refs)
        q_refs = [refs.pop(0) for _ in range(members)]
        kv_refs = [[refs.pop(0) for _ in range(members)] for _ in range(n_kv)]
        old = [refs.pop(0) for _ in range(3)] if state is not None else None
        if finish is not None:
            lam_ref, gain_ref = refs.pop(0), refs.pop(0)
            outs = [[refs.pop(0) for _ in range(2)] for _ in range(members)]
            done_tile = refs.pop()
            top, norm, acc = refs[-3:]
            refs = refs[:-3]
        else:
            top, norm, acc = [refs.pop(0) for _ in range(3)]
        queries, keyvals, q_sems, kv_sems = refs
        step = pl.program_id(0)

        def place(d):
            slot = lax.rem(sc[MEM] + members - d, members)
            return pl.ds(pl.multiple_of(slot * rows, 16), rows)

        def query_copy(d):
            return pltpu.make_async_copy(
                q_refs[d].at[:, pl.ds(0, QK)], queries.at[place(d)], q_sems.at[d]
            )

        def kv_copy(b, d):
            return pltpu.make_async_copy(
                kv_refs[b][d].at[:, pl.ds(blocks[b][1], QK + VALUE)],
                keyvals.at[b, place(d)],
                kv_sems.at[b, d],
            )

        @pl.when(step == 0)
        def _():
            for d in range(members):
                query_copy(d).start()
            for b in range(n_kv):
                @pl.when(sc[PLANE] >= blocks[b][0])
                def _():
                    for d in range(members):
                        kv_copy(b, d).start()
            for d in range(members):
                query_copy(d).wait()

        if state is not None:
            top[...] = old[0][...]
            norm[...] = old[1][...]
            acc[...] = old[2][...]

        for b in range(n_kv):
            distance = blocks[b][0]
            fresh = state is None and b == 0

            @pl.when(sc[PLANE] >= distance)
            def _():
                @pl.when(step == 0)
                def _():
                    for d in range(members):
                        kv_copy(b, d).wait()

                q_tile = queries[pl.ds(pl.multiple_of(step * tile, 16), tile), :]
                for m in range(MAPS):
                    columns = slice(m * HEAD, (m + 1) * HEAD)
                    scores = lax.dot_general(
                        q_tile[:, columns],
                        keyvals[b, :, columns],
                        (((1,), (1,)), ((), ())),
                        preferred_element_type=jnp.float32,
                    )
                    if distance == 0:
                        shape = (tile, plane_rows)
                        q_pos = step * tile + lax.broadcasted_iota(jnp.int32, shape, 0)
                        k_pos = lax.broadcasted_iota(jnp.int32, shape, 1)
                        scores = jnp.where(k_pos <= q_pos, scores, very_low)
                    best = jnp.max(scores, axis=-1, keepdims=True)
                    if not fresh:
                        before = top[m, :, :1]
                        best = jnp.maximum(best, before)
                    weights = jnp.exp2((scores - best) * scale)
                    sums = jnp.sum(weights, axis=-1, keepdims=True)
                    product = jnp.dot(
                        weights.astype(jnp.bfloat16),
                        keyvals[b, :, QK:],
                        preferred_element_type=jnp.float32,
                    )
                    if not fresh:
                        factor = jnp.exp2((before - best) * scale)
                        sums = sums + norm[m, :, :1] * factor
                        product = product + acc[m] * factor
                    top[m] = jnp.broadcast_to(best, (tile, 128))
                    norm[m] = jnp.broadcast_to(sums, (tile, 128))
                    acc[m] = product

        if finish is not None:
            lam = lam_ref[sc[MEM]]
            combined = acc[0] / norm[0, :, :1] - lam * acc[1] / norm[1, :, :1]
            mean = jnp.mean(combined * combined, axis=-1, keepdims=True)
            normed = combined * lax.rsqrt(mean + norm_floor) * gain_ref[...]
            done_tile[...] = normed.astype(jnp.bfloat16)
            per_member = rows // tile
            owner = step // per_member
            chip = lax.rem(step, per_member)
            part = tile // 2
            for d in range(members):

                @pl.when(lax.rem(sc[MEM] + d, members) == owner)
                def _():
                    for e in range(2):
                        core = jnp.bitwise_xor(sc[CORE], e)
                        take = pl.ds(pl.multiple_of(core * part, 16), part)
                        put = pl.ds(pl.multiple_of(chip * part, 16), part)
                        outs[d][e][put, :] = done_tile[take, :]

    any_spec = pl.BlockSpec(memory_space=pl.ANY)
    small = pl.BlockSpec((MAPS, tile, 128), lambda i, sc: (0, i, 0))
    large = pl.BlockSpec((MAPS, tile, VALUE), lambda i, sc: (0, i, 0))
    operands = list(query_parts) + [part for block in blocks for part in block[2]]
    in_specs = [any_spec] * len(operands)
    if state is not None:
        operands += list(state)
        in_specs += [small, small, large]
    scratch = [
        pltpu.VMEM((plane_rows, QK), jnp.bfloat16),
        pltpu.VMEM((n_kv, plane_rows, QK + VALUE), jnp.bfloat16),
        pltpu.SemaphoreType.DMA((members,)),
        pltpu.SemaphoreType.DMA((n_kv, members)),
    ]
    if finish is not None:
        lambdas, gain = finish
        operands += [lambdas, gain]
        in_specs += [
            pl.BlockSpec(memory_space=pltpu.SMEM),
            pl.BlockSpec(gain.shape, lambda i, sc: (0, 0)),
        ]
        shape = (rows // 2, VALUE)
        out_shape = [jax.ShapeDtypeStruct(shape, jnp.bfloat16)] * (2 * members)
        out_specs = [pl.BlockSpec(shape, lambda i, sc: (0, 0))] * (2 * members)
        scratch += [
            pltpu.VMEM((MAPS, tile, 128), jnp.float32),
            pltpu.VMEM((MAPS, tile, 128), jnp.float32),
            pltpu.VMEM((MAPS, tile, VALUE), jnp.float32),
            pltpu.VMEM((tile, VALUE), jnp.bfloat16),
        ]
    else:
        out_shape = [
            jax.ShapeDtypeStruct((MAPS, plane_rows, 128), jnp.float32),
            jax.ShapeDtypeStruct((MAPS, plane_rows, 128), jnp.float32),
            jax.ShapeDtypeStruct((MAPS, plane_rows, VALUE), jnp.float32),
        ]
        out_specs = [small, small, large]
    return pl.pallas_call(
        kernel,
        grid_spec=pltpu.PrefetchScalarGridSpec(
            num_scalar_prefetch=1,
            grid=(plane_rows // tile,),
            in_specs=in_specs,
            out_specs=out_specs,
            scratch_shapes=scratch,
        ),
        out_shape=out_shape,
        compiler_params=pltpu.CompilerParams(vmem_limit_bytes=48 * 2**20),
        cost_estimate=pl.CostEstimate(
            flops=4 * plane_rows * plane_rows * n_kv * MAPS * (HEAD + VALUE),
            bytes_accessed=2 * plane_rows * n_kv * (QK + VALUE),
            transcendentals=n_kv * MAPS * plane_rows * plane_rows,
        ),
        name="attend",
    )(scalars, *operands)


def output_part(scalars, head_parts, weight_own, weight_twin, flip, dtype):
    rows = head_parts[0][0].shape[0] // 2
    members = len(head_parts)
    columns = weight_own.shape[1]

    def kernel(sc, *refs):
        refs = list(refs)
        parts = [[refs.pop(0) for _ in range(2)] for _ in range(members)]
        weights = [refs.pop(0), refs.pop(0)]
        out, = refs
        chip = jnp.bitwise_xor(sc[CHIP], flip)
        take = pl.ds(pl.multiple_of(chip * rows, 16), rows)
        total = jnp.zeros((rows, columns), jnp.float32)
        for d in range(members):
            head = lax.rem(sc[MEM] + members - d, members)
            for e in range(2):
                band = pl.ds(pl.multiple_of(head * VALUE, 16), VALUE)
                total = total + jnp.dot(
                    parts[d][e][take, :],
                    weights[e][band, :],
                    preferred_element_type=jnp.float32,
                )
        out[...] = total.astype(dtype)

    whole = lambda a: pl.BlockSpec(a.shape, lambda i, sc: (0, 0))
    flat = [part for pair in head_parts for part in pair]
    return pl.pallas_call(
        kernel,
        grid_spec=pltpu.PrefetchScalarGridSpec(
            num_scalar_prefetch=1,
            grid=(1,),
            in_specs=[whole(a) for a in flat + [weight_own, weight_twin]],
            out_specs=pl.BlockSpec((rows, columns), lambda i, sc: (0, 0)),
        ),
        out_shape=jax.ShapeDtypeStruct((rows, columns), dtype),
        compiler_params=pltpu.CompilerParams(vmem_limit_bytes=40 * 2**20),
        cost_estimate=pl.CostEstimate(
            flops=2 * rows * columns * 2 * weight_own.shape[0],
            bytes_accessed=4 * weight_own.size + 6 * rows * columns,
            transcendentals=0,
        ),
        name="output_part",
    )(scalars, *flat, weight_own, weight_twin)


def permuted_plan(sp_size, tp_size, activations, query_weight, key_weight, value_weight, out_weight, lambdas, head_gain):
    members = lambdas.shape[0]
    planes = sp_size // members
    member_of = lambda s: s % members
    plane_of = lambda s: s // members

    def move(array, target, least=0):
        pairs = []
        for s in range(sp_size):
            for t in range(tp_size):
                to = target(plane_of(s), member_of(s), t)
                if to is None or to[0] < least:
                    continue
                pairs.append((s * tp_size + t, (to[0] * members + to[1]) * tp_size + to[2]))
        return lax.ppermute(array, AXES, pairs)

    def upward(z, y, t):
        return (z + 1, y, t) if z + 1 < planes else None

    flip = lambda bits: lambda z, y, t: (z, y, t ^ bits)
    turn = lambda d, bits=0: lambda z, y, t: (z, (y + d) % members, t ^ bits)

    sp_index = lax.axis_index("sp").astype(jnp.int32)
    tp_index = lax.axis_index("tp").astype(jnp.int32)
    scalars = jnp.stack(
        [tp_index, sp_index % members, sp_index // members, tp_index % 2, tp_index // 2]
    )

    blocks = [activations]
    for k in range(1, planes):
        blocks.append(move(blocks[-1], upward, k))

    gathered = []
    for k, block in enumerate(blocks):
        across = move(block, flip(2), k)
        gathered.append((block, move(block, flip(1), k), across, move(across, flip(1), k)))

    def exchange(parts, k):
        return [parts[0]] + [move(parts[d], turn(d), k) for d in range(1, members)]

    own = exchange(
        project(scalars, gathered[0], [query_weight, key_weight, value_weight], members, 0), 0
    )
    keyvals = [(0, QK, own)]
    for k in range(1, planes):
        parts = project(scalars, gathered[k], [key_weight, value_weight], members, k)
        keyvals.append((k, 0, exchange(parts, k)))
    out_twin = move(out_weight, flip(1))

    state = attend(scalars, own, keyvals[:-1], None, None)
    finish = (lambdas, head_gain.reshape(1, VALUE))
    flat = attend(scalars, own, keyvals[-1:], state, finish)
    heads = [
        [move(flat[2 * d + e], turn(d, e)) if d or e else flat[0] for e in range(2)]
        for d in range(members)
    ]
    theirs = output_part(scalars, heads, out_weight, out_twin, 1, jnp.bfloat16)
    arrived = move(theirs, flip(2))
    mine = output_part(scalars, heads, out_weight, out_twin, 0, jnp.float32)
    return (mine + arrived.astype(jnp.float32)).astype(jnp.bfloat16)


def solution(mesh):
    in_specs = (
        P(("sp", "tp"), None),
        P(None, "tp"),
        P(None, "tp"),
        P(None, "tp"),
        P("tp", None),
        P("tp"),
        P(),
    )
    out_specs = P(("sp", "tp"), None)
    sp_size, tp_size = mesh.shape["sp"], mesh.shape["tp"]

    def shards(*arrays):
        members = arrays[5].shape[0]
        planes = sp_size // members
        if tp_size == 4 and members == 2 and sp_size % members == 0 and planes <= 8:
            return permuted_plan(sp_size, tp_size, *arrays)
        return gathered_plan(*arrays)

    return jax.shard_map(shards, mesh=mesh, in_specs=in_specs, out_specs=out_specs, check_vma=False)
```
